32 devices in a mesh: sp: 8 (over z, core), tp: 4 (over y, x).
Axes of the slice: x: 2, y: 2, z: 4, core: 2. Of those that a mesh axis runs over, the one named last changes fastest.
Arguments:
- moe_input: bfloat16 [1024, 2048], P('sp', 'tp'), may hold values from -6 to 6
- cotangent: bfloat16 [1024, 2048], P('sp', 'tp'), may hold values from -6 to 6
- routes: int32 [1024, 2], P('sp'), may hold values from 0 to 7, all different within a row; in each aligned block of 128 rows (0 to 127, 128 to 255, ...) at most 40 rows name the same one
- route_weights: float32 [1024, 2], P('sp'), may hold values from 0.2 to 1
- gate_branch: bfloat16 [1024, 2560], P('sp', 'tp'), may hold values from -6 to 6
- log_decay: float32 [1024, 2560], P('sp', 'tp'), may hold values from -0.12 to 0
- states: float32 [1024, 2560], P('sp', 'tp'), may hold values from -6 to 6
- w_gate: bfloat16 [8, 2048, 2048], P('sp', None, 'tp'), may hold values from -0.125 to 0.125
- w_up: bfloat16 [8, 2048, 2048], P('sp', None, 'tp'), may hold values from -0.125 to 0.125
- w_down: bfloat16 [8, 2048, 2048], P('sp', 'tp'), may hold values from -0.125 to 0.125
- out_proj: bfloat16 [2048, 2560], P('sp', 'tp'), may hold values from -0.125 to 0.125
Outputs:
- grad_w_gate: float32 [8, 2048, 2048], P('sp', None, 'tp')
- grad_w_up: float32 [8, 2048, 2048], P('sp', None, 'tp')
- grad_w_down: float32 [8, 2048, 2048], P('sp', 'tp')
- grad_out_proj: float32 [2048, 2560], P('sp', 'tp')
- grad_gate_branch: bfloat16 [1024, 2560], P('sp', 'tp')
- grad_log_decay: bfloat16 [1024, 2560], P('sp', 'tp')
- grad_input_term: float32 [1024, 2560], P('sp', 'tp')
The draws below stay inside these ranges and needn't reach their ends.
Inputs may be any that keep to these rules, and one draw needn't show every extreme that they name: `routes`: in the rows of one device no expert is named by more than 40 entries, and in every draw some expert is named by exactly 40 entries of one device's rows.
All inputs are finite; a program needn't handle non-finite values.
Results may differ from the reference program's by a relative error of at most 0.025.
Values may be sent and summed in bfloat16 or wider, within the bound.
A program may use at most 64 MiB of HBM per device.

```python
import math
import jax
import jax.numpy as jnp
import numpy as np
from jax import lax

D = 2048
W = 2560
F = 2048
TOP = 2
TOK_DEV = 128
EXPERTS = 8
TOKENS = 1024
CAP = 40
N_SP = 8
N_TP = 4


def draw_log_decay(key, part):
    key_kind, key_rate, key_block, key_cell = jax.random.split(key, 4)
    slow_share = 50
    slow_mask = jax.random.randint(key_kind, (W,), 0, 100) < slow_share
    slow_rate = jax.random.uniform(key_rate, (W,), jnp.float32, 0.3, 0.5) * math.log(10.0) / TOKENS
    fast_rate = jax.random.uniform(jax.random.fold_in(key_rate, 7), (W,), jnp.float32, 1.0 / 60.0, 1.0 / 25.0)
    chan_rates = jnp.where(slow_mask, slow_rate, fast_rate)
    block_scale = jnp.exp(jax.random.uniform(key_block, (TOKENS // TOK_DEV, W), jnp.float32, -math.log(2.0), math.log(2.0)))
    block_scale = jnp.repeat(block_scale, TOK_DEV, axis=0)
    cell_scale = jax.random.uniform(key_cell, (TOKENS, W), jnp.float32, 0.5, 1.5)
    return -(chan_rates[None, :] * block_scale * cell_scale)


def strengthened(entries, rng, source, target, blocks, factor):
    owner, partner = [(jnp.arange(entries.shape[position]) // (entries.shape[position] // blocks)).reshape([-1 if axis == position else 1 for axis in range(entries.ndim)]) for position in (source, target)]
    chosen = jax.random.permutation(rng, blocks)[partner]
    strong = (owner == chosen) | (owner == (partner + blocks // 2) % blocks)
    return jnp.where(strong, factor * entries, entries)


def shard_levels(key, dims, cuts, smallest, largest):
    loudness, own = 1.0, jax.random.fold_in(key, 6)
    for dim, blocks in cuts:
        heights = jnp.exp(jax.random.uniform(jax.random.fold_in(own, dim), (blocks,), jnp.float32, smallest / len(cuts), largest / len(cuts)))
        loudness = loudness * jnp.repeat(heights, dims[dim] // blocks).reshape([-1 if axis == dim else 1 for axis in range(len(dims))])
    return loudness


def deal_out(own_key, own, number, rows, count, top, bound, lean):
    ranking = jax.random.permutation(own_key, count)
    heavy_load, ordinary = load_shares(count, rows * top, bound, lean, True), load_shares(count, rows * top, bound, lean, False)
    places = jnp.arange(count)

    def named(lengths, turn):
        used = int((lengths > 0).sum())
        fixed = max(1, used // 4)
        moved = fixed + (places - fixed + turn * (used - fixed)) % max(1, count - fixed)
        return jnp.zeros((count,), jnp.int32).at[ranking[jnp.where(places < fixed, places, moved)]].set(jnp.asarray(lengths, jnp.int32))

    lengths = jnp.where(number % 4 == 0, named(heavy_load, number // 4), named(ordinary, number - number // 4 - 1))
    mixed = jax.random.permutation(jax.random.fold_in(own, 3), count)
    source_of, taker = mixed[0:count // 2 * 2:2], mixed[1:count // 2 * 2:2]
    slack = jnp.minimum(lengths[source_of] - 1, bound - lengths[taker]) // 2
    slack = jnp.where((source_of == ranking[0]) | (taker == ranking[0]) | (lengths[taker] == 0), 0, jnp.maximum(slack, 0))
    moved = jax.random.randint(jax.random.fold_in(own, 4), (count // 2,), 0, 1 << 20) % (slack + 1)
    lengths = lengths.at[source_of].add(-moved).at[taker].add(moved)
    items = jnp.searchsorted(jnp.cumsum(lengths), jnp.arange(rows * top), side="right").astype(jnp.int32)
    listing = items.reshape(top, rows).T
    listing = listing[jax.random.permutation(jax.random.fold_in(own, 1), rows)]
    turn = jax.random.randint(jax.random.fold_in(own, 2), (rows, 1), 0, top)
    return jnp.take_along_axis(listing, (jnp.arange(top)[None, :] + turn) % top, axis=1)


def load_shares(amount, total, limit, skew, full):
    weights = [(1 << 20) // math.isqrt(standing ** skew) + 1 for standing in range(1, amount + 1)]
    largest = limit if full else min(limit, max(-(-total // amount), total * weights[0] // sum(weights)))
    least = 1 if total - largest >= amount - 1 else 0
    counts, spare = [largest] + [least] * (amount - 1), total - largest - least * (amount - 1)
    while spare > 0:
        free = [i for i in range(1, amount) if counts[i] < largest] or [i for i in range(1, amount) if counts[i] < limit]
        whole, budget = sum([weights[i] for i in free]), spare
        for i in free:
            extra = min(limit - counts[i], max(1, budget * weights[i] // whole), spare)
            counts[i] = counts[i] + extra
            spare = spare - extra
    return np.array(counts)


def gaussian(stream_key, shape, width, bound, cuts=(), kind=jnp.bfloat16):
    result = width * jax.random.normal(stream_key, shape, jnp.float32)
    if cuts:
        result = result * shard_levels(stream_key, shape, cuts, -0.22, 0.18)
    return jnp.clip(result, -bound, bound).astype(kind)


def noise_with(key, shape, deviation, reach, cuts, heavy, kind=jnp.bfloat16):
    result = deviation * jax.random.normal(key, shape, jnp.float32)
    if cuts:
        result = result * shard_levels(key, shape, cuts, -0.22, 0.18)
    return jnp.clip(strengthened(result, jax.random.fold_in(key, 3), *heavy), -reach, reach).astype(kind)


def setup_inputs(seed: int = 0) -> dict:
    key_list = jax.random.split(jax.random.key(seed), 12)
    moe_input = gaussian(key_list[0], (TOKENS, D), 1.0, 6.0, ((0, 8), (1, 4)))
    cotangent = noise_with(key_list[1], (TOKENS, D), 1.0, 6.0, ((0, 8), (1, 4)), (0, 1, 8, 2.0))
    routes_keys = jax.random.split(jax.random.fold_in(key_list[2], 1), TOKENS // TOK_DEV)
    routes_turns = jax.random.permutation(jax.random.fold_in(key_list[2], 3), TOKENS // TOK_DEV)
    routes = jax.vmap(lambda own, number: deal_out(jax.random.fold_in(key_list[2], 2), own, number, TOK_DEV, EXPERTS, TOP, CAP, 2))(routes_keys, routes_turns).reshape((TOKENS, TOP))
    route_weights = jnp.clip(0.2 + 0.8 * jax.random.uniform(key_list[3], (TOKENS, TOP), jnp.float32) ** shard_levels(key_list[3], (TOKENS, TOP), ((0, 8),), -0.2, 0.2), 0.2, 1.0)
    gate_branch = gaussian(key_list[4], (TOKENS, W), 1.0, 6.0, ((0, 8), (1, 4)))
    log_decay = draw_log_decay(jax.random.fold_in(key_list[11], 71), 0)
    states = gaussian(key_list[6], (TOKENS, W), 1.0, 6.0, ((0, 8), (1, 4)), jnp.float32)
    w_gate = gaussian(key_list[7], (EXPERTS, D, F), D ** -0.5, 0.125, ((0, 8), (2, 4)))
    w_up = gaussian(key_list[8], (EXPERTS, D, F), D ** -0.5, 0.125, ((0, 8), (2, 4)))
    w_down = gaussian(key_list[9], (EXPERTS, F, D), F ** -0.5, 0.125, ((0, 8), (1, 4)))
    out_proj = gaussian(key_list[10], (D, W), W ** -0.5, 0.125, ((0, 8), (1, 4)))
    return dict(moe_input=moe_input, cotangent=cotangent, routes=routes, route_weights=route_weights, gate_branch=gate_branch, log_decay=log_decay, states=states, w_gate=w_gate, w_up=w_up, w_down=w_down, out_proj=out_proj)


def silu_parts(pre_gate):
    sigmoid_val = jax.nn.sigmoid(pre_gate)
    return (pre_gate * sigmoid_val, sigmoid_val * (1.0 + pre_gate * (1.0 - sigmoid_val)))

def combine_pair(left_pair, right_pair):
    return (left_pair[0] * right_pair[0], right_pair[0] * left_pair[1] + right_pair[1])

def expert_backward(row_data, scaled, gate_w, up_w, down_w):
    pre_gate = jnp.dot(row_data, gate_w, preferred_element_type=jnp.float32)
    pre_up = jnp.dot(row_data, up_w, preferred_element_type=jnp.float32)
    active, slope = silu_parts(pre_gate)
    hidden = (active * pre_up).astype(jnp.bfloat16)
    grad_down = jnp.dot(hidden.T, scaled, preferred_element_type=jnp.float32)
    grad_hidden = jnp.dot(scaled, down_w.T, preferred_element_type=jnp.float32)
    grad_pre_gate = (grad_hidden * pre_up * slope).astype(jnp.bfloat16)
    grad_pre_up = (grad_hidden * active).astype(jnp.bfloat16)
    grad_gate_w = jnp.dot(row_data.T, grad_pre_gate, preferred_element_type=jnp.float32)
    grad_up_w = jnp.dot(row_data.T, grad_pre_up, preferred_element_type=jnp.float32)
    row_total = grad_pre_gate.shape[0]
    blocked_gate = grad_pre_gate.reshape(row_total, N_TP, F // N_TP).astype(jnp.float32)
    blocked_up = grad_pre_up.reshape(row_total, N_TP, F // N_TP).astype(jnp.float32)
    weight_gate = gate_w.reshape(D, N_TP, F // N_TP).astype(jnp.float32)
    weight_up = up_w.reshape(D, N_TP, F // N_TP).astype(jnp.float32)
    block_terms = jnp.einsum('nbf,dbf->bnd', blocked_gate, weight_gate) + jnp.einsum('nbf,dbf->bnd', blocked_up, weight_up)
    rounded = lax.optimization_barrier(block_terms.astype(jnp.bfloat16))
    entry_grad = lax.optimization_barrier(jnp.sum(rounded.astype(jnp.float32), axis=0)).astype(jnp.bfloat16)
    return (grad_gate_w, grad_up_w, grad_down, entry_grad)

def reference(moe_input, cotangent, routes, route_weights, gate_branch, log_decay, states, w_gate, w_up, w_down, out_proj):
    flat_routes = routes.reshape(-1).astype(jnp.int32)
    flat_weights = route_weights.reshape(-1)
    owners = jnp.arange(TOKENS * TOP, dtype=jnp.int32) // TOP
    room = N_SP * CAP

    def per_expert(totals, inputs):
        expert, gate_w, up_w, down_w = inputs
        sorted_idx = jnp.argsort((flat_routes != expert).astype(jnp.int32), stable=True)[:room].astype(jnp.int32)
        live_rows = (flat_routes[sorted_idx] == expert).astype(jnp.float32)
        token_idx = owners[sorted_idx]
        row_data = moe_input[token_idx]
        scaled = ((live_rows * flat_weights[sorted_idx])[:, None] * cotangent[token_idx].astype(jnp.float32)).astype(jnp.bfloat16)
        grad_gate_w, grad_up_w, grad_down, entry_grad = expert_backward(row_data, scaled, gate_w, up_w, down_w)
        totals = totals.at[token_idx].add(entry_grad.astype(jnp.float32) * live_rows[:, None])
        return (totals, (grad_gate_w, grad_up_w, grad_down))
    totals, grads = lax.scan(per_expert, jnp.zeros((TOKENS, D), jnp.float32), (jnp.arange(EXPERTS, dtype=jnp.int32), w_gate, w_up, w_down))
    grad_w_gate, grad_w_up, grad_w_down = grads
    grad_tokens = (cotangent.astype(jnp.float32) + totals).astype(jnp.bfloat16)
    active_gate, pullback = jax.vjp(jax.nn.gelu, gate_branch.astype(jnp.float32))
    mixed_in = (active_gate * states).astype(jnp.bfloat16)
    grad_out_proj = jnp.dot(grad_tokens.T, mixed_in, preferred_element_type=jnp.float32)
    grad_mixed = jnp.dot(grad_tokens, out_proj, preferred_element_type=jnp.float32)
    grad_gate_branch = pullback(grad_mixed * states)[0].astype(jnp.bfloat16)
    grad_state = grad_mixed * active_gate
    decays = jnp.exp(log_decay)
    next_decay = jnp.concatenate([decays[1:], jnp.zeros_like(decays[:1])], axis=0)
    _, back_flip = lax.associative_scan(combine_pair, (jnp.flip(next_decay, 0), jnp.flip(grad_state, 0)))
    grad_input_term = jnp.flip(back_flip, 0)
    prev_states = jnp.concatenate([jnp.zeros_like(states[:1]), states[:-1]], axis=0)
    grad_log_decay = (grad_input_term * decays * prev_states).astype(jnp.bfloat16)
    return (grad_w_gate, grad_w_up, grad_w_down, grad_out_proj, grad_gate_branch, grad_log_decay, grad_input_term)
```

```python
import jax
import jax.numpy as jnp
from jax import lax
from jax.experimental import pallas as pl
from jax.experimental.pallas import tpu as pltpu
from jax.sharding import PartitionSpec as P

BF = jnp.bfloat16
F32 = jnp.float32
CORES = 2
GELU_C = 0.7978845608028654
GELU_A = 0.044715


def silu_parts(pre_gate):
    sigmoid_val = jax.nn.sigmoid(pre_gate)
    return (pre_gate * sigmoid_val, sigmoid_val * (1.0 + pre_gate * (1.0 - sigmoid_val)))


def contract_rows(left_mat, right_mat):
    return lax.dot_general(
        left_mat, right_mat, (((0,), (0,)), ((), ())), preferred_element_type=F32
    )


def contract_cols(left_mat, right_mat):
    return lax.dot_general(
        left_mat, right_mat, (((1,), (1,)), ((), ())), preferred_element_type=F32
    )


def gelu_parts(x):
    t = jnp.tanh(GELU_C * (x + GELU_A * (x * x * x)))
    half = 0.5 * (1.0 + t)
    slope = half + 0.5 * x * (1.0 - t * t) * (GELU_C * (1.0 + 3.0 * GELU_A * x * x))
    return x * half, slope


def selection(routes_t, weights_t, groups, room):
    picks, toks = routes_t.shape
    experts = lax.broadcasted_iota(jnp.int32, (groups, toks), 0)
    named = jnp.zeros((groups, toks), F32)
    weight = jnp.zeros((groups, toks), F32)
    for k in range(picks):
        hit = routes_t[k : k + 1, :] == experts
        named = named + jnp.where(hit, 1.0, 0.0)
        weight = weight + jnp.where(hit, weights_t[k : k + 1, :], 0.0)
    rows = lax.broadcasted_iota(jnp.int32, (toks, toks), 0)
    cols = lax.broadcasted_iota(jnp.int32, (toks, toks), 1)
    before = jnp.where(rows < cols, 1.0, 0.0).astype(BF)
    slot = jnp.dot(named.astype(BF), before, preferred_element_type=F32)
    slot = jnp.where(named > 0.5, slot, -1.0)
    place = lax.broadcasted_iota(jnp.int32, (room, toks), 0).astype(F32)
    picked, column = [], []
    for e in range(groups):
        one = jnp.where(slot[e : e + 1, :] == place, 1.0, 0.0)
        picked.append(one)
        column.append(jnp.sum(one * weight[e : e + 1, :], axis=1, keepdims=True))
    return jnp.concatenate(picked, axis=0).astype(BF), jnp.concatenate(column, axis=0)


def greet(groups, parts, mine, col):
    barrier = pltpu.get_barrier_semaphore()
    for d in range(1, groups):
        pl.semaphore_signal(
            barrier, inc=1, device_id={"sp": lax.rem(mine + d, groups)},
            device_id_type=pl.DeviceIdType.MESH,
        )
    for d in range(1, parts):
        pl.semaphore_signal(
            barrier, inc=1, device_id={"tp": lax.rem(col + d, parts)},
            device_id_type=pl.DeviceIdType.MESH,
        )
    pl.semaphore_wait(barrier, groups + parts - 2)


def remote(src, dst, send, recv, axis, peer):
    return pltpu.make_async_remote_copy(
        src_ref=src, dst_ref=dst, send_sem=send, recv_sem=recv,
        device_id={axis: peer}, device_id_type=pl.DeviceIdType.MESH,
    )


def dispatch_kernel(
    groups, parts, room,
    x_ref, cot_ref, routes_ref, weights_ref, gate_ref, states_ref, proj_ref,
    rows_ref, scaled_ref, proj_all, mixed_all,
    out_x, out_c, in_x, in_c, mix_own,
    a_send, a_recv, t_send, t_recv, z_send, z_recv, c_send, c_recv, l_sem,
):
    mine, col = lax.axis_index("sp"), lax.axis_index("tp")
    width = x_ref.shape[1]
    depth = groups // CORES
    z, core = mine // CORES, lax.rem(mine, CORES)
    picked, weight = selection(routes_ref[...], weights_ref[...], groups, room)
    got = jnp.dot(picked, x_ref[...], preferred_element_type=F32).astype(BF)
    got_c = jnp.dot(picked, cot_ref[...], preferred_element_type=F32)
    got_c = (got_c * weight).astype(BF)
    for e in range(groups):
        out_x[e] = got[e * room : (e + 1) * room]
        out_c[e] = got_c[e * room : (e + 1) * room]
    act, _ = gelu_parts(gate_ref[...].astype(F32))
    mix_own[...] = (act * states_ref[...]).astype(BF)
    greet(groups, parts, mine, col)

    waits = []
    own = []
    for a, (src, dst) in enumerate(((out_x, in_x), (out_c, in_c))):
        for d in range(1, groups):
            peer = lax.rem(mine + d, groups)
            c = remote(src.at[peer], dst.at[mine], a_send.at[a, d], a_recv.at[a, d], "sp", peer)
            c.start()
            waits.append(c)
        o = pltpu.make_async_copy(src.at[mine], dst.at[mine], l_sem.at[a])
        o.start()
        own.append(o)
    for a, (src, dst) in enumerate(((mix_own, mixed_all), (proj_ref, proj_all))):
        o = pltpu.make_async_copy(src, dst.at[mine], l_sem.at[2 + a])
        o.start()
        own.append(o)
    own[2].wait()
    own[3].wait()

    pairs = (mixed_all, proj_all)

    def chain(step, wait):
        for a, buf in enumerate(pairs):
            right = buf.at[jnp.maximum(z - step, 0) * CORES + core]
            left = buf.at[jnp.minimum(z + step, depth - 1) * CORES + core]
            go_r = jnp.logical_and(z - step >= 0, z + 1 < depth)
            go_l = jnp.logical_and(z + step < depth, z >= 1)
            up = jnp.minimum(z + 1, depth - 1) * CORES + core
            down = jnp.maximum(z - 1, 0) * CORES + core

            def c_r():
                return remote(right, right, z_send.at[a, 0, step], z_recv.at[a, 0, step], "sp", up)

            def c_l():
                return remote(left, left, z_send.at[a, 1, step], z_recv.at[a, 1, step], "sp", down)

            @pl.when(go_r)
            def _():
                c_r().wait_send() if wait else c_r().start()

            @pl.when(go_l)
            def _():
                c_l().wait_send() if wait else c_l().start()

    def arrived(step):
        for a, buf in enumerate(pairs):
            from_l = buf.at[jnp.maximum(z - 1 - step, 0) * CORES + core]
            from_r = buf.at[jnp.minimum(z + 1 + step, depth - 1) * CORES + core]
            for way, ok, ref in (
                (0, z - 1 - step >= 0, from_l),
                (1, z + 1 + step < depth, from_r),
            ):
                @pl.when(ok)
                def _(way=way, ref=ref, a=a):
                    remote(ref, ref, z_send.at[a, way, step], z_recv.at[a, way, step],
                           "sp", lax.rem(mine + 1, groups)).wait_recv()

    partner = z * CORES + (1 - core)

    def across(step, way, mode):
        for a, buf in enumerate(pairs):
            ok = z - step >= 0 if way == 0 else z + step < depth
            zz = jnp.maximum(z - step, 0) if way == 0 else jnp.minimum(z + step, depth - 1)
            ref = buf.at[zz * CORES + (1 - core if mode == "recv" else core)]

            @pl.when(ok)
            def _():
                c = remote(ref, ref, c_send.at[a, way, step], c_recv.at[a, way, step], "sp", partner)
                if mode == "start":
                    c.start()
                elif mode == "send":
                    c.wait_send()
                else:
                    c.wait_recv()

    chain(0, False)
    across(0, 0, "start")

    tp_waits = []
    here = pl.ds(pl.multiple_of(col * width, width), width)
    for a, (src, dst) in enumerate(((in_x, rows_ref), (in_c, scaled_ref))):
        own[a].wait()
        for c in waits[a * (groups - 1) : (a + 1) * (groups - 1)]:
            c.wait_recv()
        for d in range(1, parts):
            c = remote(src, dst.at[:, :, here], t_send.at[a, d], t_recv.at[a, d], "tp",
                       lax.rem(col + d, parts))
            c.start()
            tp_waits.append(c)
        o = pltpu.make_async_copy(src, dst.at[:, :, here], l_sem.at[4 + a])
        o.start()
        own.append(o)
    for step in range(depth - 1):
        arrived(step)
        if step + 1 < depth - 1:
            chain(step + 1, False)
        across(step + 1, 0, "start")
        across(step + 1, 1, "start")
    for c in waits:
        c.wait_send()
    for c in tp_waits:
        c.wait()
    own[4].wait()
    own[5].wait()
    for step in range(depth - 1):
        chain(step, True)
    for step in range(depth):
        for way in range(2):
            if step == 0 and way == 1:
                continue
            across(step, way, "send")
            across(step, way, "recv")


def finish_kernel(
    groups, parts, room,
    terms_ref, cot_ref, routes_ref, weights_ref, gate_ref, states_ref, decay_ref, proj_ref, mixed_ref,
    outp_ref, ggate_ref, gdecay_ref, gin_ref,
    shares, summed, back, flipped, blocks, carry_own, carry_in, prev_in,
    s_send, s_recv, a_send, a_recv, g_send, g_recv, b_send, b_recv, k_send, k_recv, p_send, p_recv, l_sem,
):
    mine, col = lax.axis_index("sp"), lax.axis_index("tp")
    toks, width = cot_ref.shape
    greet(groups, parts, mine, col)

    def near(width_of, index):
        return pl.ds(pl.multiple_of(index * width_of, width_of), width_of)

    nxt = lax.rem(mine + 1, groups)
    prev_copy = remote(states_ref.at[pl.ds(toks - 8, 8)], prev_in, p_send, p_recv, "sp", nxt)
    share_copies = []
    for d in range(1, parts):
        peer = lax.rem(col + d, parts)
        c = remote(terms_ref.at[:, :, near(width, peer)], shares.at[d - 1], s_send.at[d], s_recv.at[d],
                   "tp", peer)
        c.start()
        share_copies.append(c)
    prev_copy.start()
    picked, _ = selection(routes_ref[...], weights_ref[...], groups, room)
    rows = lax.broadcasted_iota(jnp.int32, (toks, toks), 0)
    cols = lax.broadcasted_iota(jnp.int32, (toks, toks), 1)
    eye = jnp.where(rows == cols, 1.0, 0.0).astype(BF)
    act, slope = gelu_parts(gate_ref[...].astype(F32))
    decays = jnp.exp(decay_ref[...])
    for c in share_copies:
        c.wait_recv()
    for g in range(groups):
        total = terms_ref[g, :, near(width, col)].astype(F32)
        for d in range(1, parts):
            total = total + shares[d - 1, g].astype(F32)
        summed[g] = total.astype(BF)
    back_copies = []
    for d in range(1, groups):
        peer = lax.rem(mine + d, groups)
        c = remote(summed.at[peer], back.at[mine], a_send.at[d], a_recv.at[d], "sp", peer)
        c.start()
        back_copies.append(c)
    o = pltpu.make_async_copy(summed.at[mine], back.at[mine], l_sem.at[0])
    o.start()
    o.wait()
    for c in back_copies:
        c.wait_recv()
    total = contract_rows(cot_ref[...], eye)
    for g in range(groups):
        total = total + contract_rows(back[g], picked[g * room : (g + 1) * room])
    flipped[near(width, col), :] = total.astype(BF)
    grad_copies = []
    for d in range(1, parts):
        part = flipped.at[near(width, col)]
        c = remote(part, part, g_send.at[d], g_recv.at[d], "tp", lax.rem(col + d, parts))
        c.start()
        grad_copies.append(c)
    for c in grad_copies:
        c.wait_recv()
    high = flipped.shape[0] // groups
    block_copies = []
    for d in range(1, groups):
        peer = lax.rem(mine + d, groups)
        c = remote(flipped.at[near(high, peer)], blocks.at[mine], b_send.at[d], b_recv.at[d], "sp", peer)
        c.start()
        block_copies.append(c)
    o = pltpu.make_async_copy(flipped.at[near(high, mine)], blocks.at[mine], l_sem.at[1])
    o.start()
    grad_mixed = contract_rows(flipped[...], proj_ref[...])
    states = states_ref[...]
    ggate_ref[...] = (grad_mixed * states * slope).astype(BF)
    local = grad_mixed * act
    line = lax.broadcasted_iota(jnp.int32, local.shape, 0)
    span = jnp.where(line < toks - 1, pltpu.roll(decays, toks - 1, 0), 1.0)
    k = 1
    while k < toks:
        inside = line < toks - k
        local = local + span * jnp.where(inside, pltpu.roll(local, toks - k, 0), 0.0)
        span = span * jnp.where(inside, pltpu.roll(span, toks - k, 0), 1.0)
        k *= 2
    eight = lax.broadcasted_iota(jnp.int32, (8, local.shape[1]), 0)
    whole = span[0:1] * decays[0:1]
    entry = local[0:1] * decays[0:1]
    carry_own[...] = jnp.where(eight == 0, whole, entry)
    carry_copies = []
    for d in range(1, groups):
        peer = lax.rem(mine + d, groups)
        c = remote(carry_own, carry_in.at[d - 1], k_send.at[d], k_recv.at[d], "sp", peer)
        c.start()
        carry_copies.append(c)
    prev_copy.wait_recv()
    first = jnp.where(mine > 0, prev_in[7:8, :], 0.0)
    prev = jnp.where(line == 0, first, pltpu.roll(states, 1, 0))
    for c in carry_copies:
        c.wait_recv()
    carried = jnp.zeros_like(whole)
    for ahead in range(groups - 1, 0, -1):
        got = carry_in[groups - ahead - 1]
        carried = jnp.where(mine + ahead < groups, got[1:2] + got[0:1] * carried, carried)
    grad_in = local + span * carried
    gin_ref[...] = grad_in
    gdecay_ref[...] = (grad_in * decays * prev).astype(BF)
    o.wait()
    for c in block_copies:
        c.wait_recv()
    total = jnp.dot(blocks[0], mixed_ref[0], preferred_element_type=F32)
    for g in range(1, groups):
        total = total + jnp.dot(blocks[g], mixed_ref[g], preferred_element_type=F32)
    outp_ref[...] = total
    for c in [prev_copy] + share_copies + back_copies + grad_copies + block_copies + carry_copies:
        c.wait_send()


def shards(
    moe_input, cotangent, routes, route_weights, gate_branch, log_decay, states,
    w_gate, w_up, w_down, out_proj,
):
    groups, parts = lax.axis_size("sp"), lax.axis_size("tp")
    tok_rows, picks = routes.shape
    width = moe_input.shape[1]
    model = width * parts
    chans = states.shape[1]
    room = tok_rows * picks * 5 // (4 * groups)
    room = (room + 7) // 8 * 8
    depth = groups // CORES
    high = out_proj.shape[0]
    routes_t, weights_t = routes.T, route_weights.T
    vmem = pl.BlockSpec(memory_space=pltpu.VMEM)
    dma = pltpu.SemaphoreType.DMA

    def kernel_of(body, name):
        def run(*refs):
            body(groups, parts, room, *refs)
        run.__name__ = name
        return run

    rows_in, cot_in, proj_all, mixed_all = pl.pallas_call(
        kernel_of(dispatch_kernel, "dispatch"),
        out_shape=[
            jax.ShapeDtypeStruct((groups, room, model), BF),
            jax.ShapeDtypeStruct((groups, room, model), BF),
            jax.ShapeDtypeStruct((groups, high, chans), BF),
            jax.ShapeDtypeStruct((groups, tok_rows, chans), BF),
        ],
        in_specs=[vmem] * 7,
        out_specs=[vmem] * 4,
        scratch_shapes=[pltpu.VMEM((groups, room, width), BF)] * 4
        + [pltpu.VMEM((tok_rows, chans), BF)]
        + [dma((2, groups))] * 2 + [dma((2, parts))] * 2
        + [dma((2, 2, depth))] * 4 + [dma((6,))],
        compiler_params=pltpu.CompilerParams(
            collective_id=0, has_side_effects=True, vmem_limit_bytes=50 * 1024 * 1024),
        name="dispatch",
    )(moe_input, cotangent, routes_t, weights_t, gate_branch, states, out_proj)

    row_data = rows_in.reshape(groups * room, model)
    scaled = cot_in.reshape(groups * room, model)
    gate_w, up_w, down_w = w_gate[0], w_up[0], w_down[0]
    pre_gate = jnp.dot(row_data, gate_w, preferred_element_type=F32)
    pre_up = jnp.dot(row_data, up_w, preferred_element_type=F32)
    active, slope = silu_parts(pre_gate)
    hidden = (active * pre_up).astype(BF)
    grad_hidden = contract_cols(scaled, down_w)
    grad_pre_gate = (grad_hidden * pre_up * slope).astype(BF)
    grad_pre_up = (grad_hidden * active).astype(BF)
    entry_terms = (contract_cols(grad_pre_gate, gate_w) + contract_cols(grad_pre_up, up_w)).astype(BF)
    grad_down = contract_rows(hidden, scaled)
    grad_gate_w = contract_rows(row_data, grad_pre_gate)
    grad_up_w = contract_rows(row_data, grad_pre_up)

    grad_out_proj, grad_gate_branch, grad_log_decay, grad_input_term = pl.pallas_call(
        kernel_of(finish_kernel, "finish"),
        out_shape=[
            jax.ShapeDtypeStruct((high, chans), F32),
            jax.ShapeDtypeStruct((tok_rows, chans), BF),
            jax.ShapeDtypeStruct((tok_rows, chans), BF),
            jax.ShapeDtypeStruct((tok_rows, chans), F32),
        ],
        in_specs=[vmem] * 9,
        out_specs=[vmem] * 4,
        scratch_shapes=[
            pltpu.VMEM((parts - 1, groups, room, width), BF),
            pltpu.VMEM((groups, room, width), BF),
            pltpu.VMEM((groups, room, width), BF),
            pltpu.VMEM((model, tok_rows), BF),
            pltpu.VMEM((groups, high, tok_rows), BF),
            pltpu.VMEM((8, chans), F32),
            pltpu.VMEM((groups - 1, 8, chans), F32),
            pltpu.VMEM((8, chans), F32),
        ]
        + [dma((parts,))] * 2 + [dma((groups,))] * 2 + [dma((parts,))] * 2
        + [dma((groups,))] * 4 + [dma(())] * 2 + [dma((2,))],
        compiler_params=pltpu.CompilerParams(
            collective_id=1, has_side_effects=True, vmem_limit_bytes=50 * 1024 * 1024),
        name="finish",
    )(
        entry_terms.reshape(groups, room, model), cotangent, routes_t, weights_t, gate_branch,
        states, log_decay, proj_all.reshape(groups * high, chans), mixed_all,
    )
    return (
        grad_gate_w[None], grad_up_w[None], grad_down[None], grad_out_proj,
        grad_gate_branch, grad_log_decay, grad_input_term,
    )


def solution(mesh):
    return jax.shard_map(
        shards,
        mesh=mesh,
        in_specs=(
            P("sp", "tp"), P("sp", "tp"), P("sp", None), P("sp", None), P("sp", "tp"),
            P("sp", "tp"), P("sp", "tp"), P("sp", None, "tp"), P("sp", None, "tp"),
            P("sp", "tp", None), P("sp", "tp"),
        ),
        out_specs=(
            P("sp", None, "tp"), P("sp", None, "tp"), P("sp", "tp", None), P("sp", "tp"),
            P("sp", "tp"), P("sp", "tp"), P("sp", "tp"),
        ),
        check_vma=False,
    )
```

```python
import jax
import jax.numpy as jnp
from jax import lax
from jax.experimental import pallas as pl
from jax.experimental.pallas import tpu as pltpu
from jax.sharding import PartitionSpec as P

BF = jnp.bfloat16
F32 = jnp.float32
CORES = 2
GELU_C = 0.7978845608028654
GELU_A = 0.044715


def silu_parts(pre_gate):
    sigmoid_val = jax.nn.sigmoid(pre_gate)
    return (pre_gate * sigmoid_val, sigmoid_val * (1.0 + pre_gate * (1.0 - sigmoid_val)))


def contract_rows(left_mat, right_mat):
    return lax.dot_general(
        left_mat, right_mat, (((0,), (0,)), ((), ())), preferred_element_type=F32
    )


def contract_cols(left_mat, right_mat):
    return lax.dot_general(
        left_mat, right_mat, (((1,), (1,)), ((), ())), preferred_element_type=F32
    )


def gelu_parts(x):
    t = jnp.tanh(GELU_C * (x + GELU_A * (x * x * x)))
    half = 0.5 * (1.0 + t)
    slope = half + 0.5 * x * (1.0 - t * t) * (GELU_C * (1.0 + 3.0 * GELU_A * x * x))
    return x * half, slope


def selection(routes_t, weights_t, groups, room):
    picks, toks = routes_t.shape
    experts = lax.broadcasted_iota(jnp.int32, (groups, toks), 0)
    named = jnp.zeros((groups, toks), F32)
    weight = jnp.zeros((groups, toks), F32)
    for k in range(picks):
        hit = routes_t[k : k + 1, :] == experts
        named = named + jnp.where(hit, 1.0, 0.0)
        weight = weight + jnp.where(hit, weights_t[k : k + 1, :], 0.0)
    rows = lax.broadcasted_iota(jnp.int32, (toks, toks), 0)
    cols = lax.broadcasted_iota(jnp.int32, (toks, toks), 1)
    before = jnp.where(rows < cols, 1.0, 0.0).astype(BF)
    slot = jnp.dot(named.astype(BF), before, preferred_element_type=F32)
    slot = jnp.where(named > 0.5, slot, -1.0)
    place = lax.broadcasted_iota(jnp.int32, (room, toks), 0).astype(F32)
    picked, column = [], []
    for e in range(groups):
        one = jnp.where(slot[e : e + 1, :] == place, 1.0, 0.0)
        picked.append(one)
        column.append(jnp.sum(one * weight[e : e + 1, :], axis=1, keepdims=True))
    return jnp.concatenate(picked, axis=0).astype(BF), jnp.concatenate(column, axis=0)


def greet(groups, parts, mine, col):
    barrier = pltpu.get_barrier_semaphore()
    for d in range(1, groups):
        pl.semaphore_signal(
            barrier, inc=1, device_id={"sp": lax.rem(mine + d, groups)},
            device_id_type=pl.DeviceIdType.MESH,
        )
    for d in range(1, parts):
        pl.semaphore_signal(
            barrier, inc=1, device_id={"tp": lax.rem(col + d, parts)},
            device_id_type=pl.DeviceIdType.MESH,
        )
    pl.semaphore_wait(barrier, groups + parts - 2)


def remote(src, dst, send, recv, axis, peer):
    return pltpu.make_async_remote_copy(
        src_ref=src, dst_ref=dst, send_sem=send, recv_sem=recv,
        device_id={axis: peer}, device_id_type=pl.DeviceIdType.MESH,
    )


def whole_kernel(
    groups, parts, room, chunked,
    routes_ref, weights_ref, x_any, cot_any, gate_any, states_any, decay_any, proj_any,
    wg_any, wu_any, wd_any,
    gg_ref, gu_ref, gd_ref, outp_ref, ggate_ref, gdecay_ref, gin_ref,
    x_ref, cot_ref, gate_ref, states_ref, decay_ref, wg, wu, wd,
    out_x, out_c, rows_x, rows_c, proj_all, mixed_all, mix_own, gg, gu, gd,
    terms, shares, summed, back, flipped, blocks, carry_own, carry_in, prev_in,
    a_send, a_recv, t_send, t_recv, z_send, z_recv, c_send, c_recv,
    s_send, s_recv, r_send, r_recv, g_send, g_recv, b_send, b_recv, k_send, k_recv, p_send, p_recv,
    l_sem, w_sem,
):
    mine, col = lax.axis_index("sp"), lax.axis_index("tp")
    toks, width = x_ref.shape
    model = rows_x.shape[2]
    depth = groups // CORES
    z, core = mine // CORES, lax.rem(mine, CORES)
    size = groups * room

    def near(width_of, index):
        return pl.ds(pl.multiple_of(index * width_of, width_of), width_of)

    loads = []
    for i, (s, t) in enumerate((
        (x_any, x_ref), (cot_any, cot_ref), (gate_any, gate_ref), (states_any, states_ref),
        (proj_any, proj_all.at[mine]), (decay_any, decay_ref),
        (wg_any.at[0], wg), (wu_any.at[0], wu), (wd_any.at[0], wd),
    )):
        o = pltpu.make_async_copy(s, t, l_sem.at[i])
        o.start()
        loads.append(o)

    picked, weight = selection(routes_ref[...], weights_ref[...], groups, room)
    loads[0].wait()
    got = jnp.dot(picked, x_ref[...], preferred_element_type=F32).astype(BF)
    for e in range(groups):
        out_x[e] = got[e * room : (e + 1) * room]
    loads[1].wait()
    got_c = jnp.dot(picked, cot_ref[...], preferred_element_type=F32)
    got_c = (got_c * weight).astype(BF)
    for e in range(groups):
        out_c[e] = got_c[e * room : (e + 1) * room]
    greet(groups, parts, mine, col)

    here = near(width, col)
    sends, own = [], []
    arrivals = [[None] * groups for _ in range(2)]
    for a, (src, dst) in enumerate(((out_x, rows_x), (out_c, rows_c))):
        for d in range(1, groups):
            peer = lax.rem(mine + d, groups)
            c = remote(src.at[peer], dst.at[mine, :, here], a_send.at[a, d], a_recv.at[a, d], "sp", peer)
            c.start()
            arrivals[a][d] = c
            sends.append(c)
        o = pltpu.make_async_copy(src.at[mine], dst.at[mine, :, here], w_sem.at[a])
        o.start()
        own.append(o)

    pairs = (proj_all, mixed_all)

    def chain(a, step, wait=False):
        buf = pairs[a]
        right = buf.at[jnp.maximum(z - step, 0) * CORES + core]
        left = buf.at[jnp.minimum(z + step, depth - 1) * CORES + core]
        up = jnp.minimum(z + 1, depth - 1) * CORES + core
        down = jnp.maximum(z - 1, 0) * CORES + core
        for way, ref, peer, ok in (
            (0, right, up, jnp.logical_and(z - step >= 0, z + 1 < depth)),
            (1, left, down, jnp.logical_and(z + step < depth, z >= 1)),
        ):
            @pl.when(ok)
            def _(way=way, ref=ref, peer=peer):
                c = remote(ref, ref, z_send.at[a, way, step], z_recv.at[a, way, step], "sp", peer)
                c.wait_send() if wait else c.start()

    partner = z * CORES + (1 - core)

    def across(a, step, way, mode):
        ok = z - step >= 0 if way == 0 else z + step < depth
        zz = jnp.maximum(z - step, 0) if way == 0 else jnp.minimum(z + step, depth - 1)
        ref = pairs[a].at[zz * CORES + (1 - core if mode == "recv" else core)]

        @pl.when(ok)
        def _():
            c = remote(ref, ref, c_send.at[a, way, step], c_recv.at[a, way, step], "sp", partner)
            if mode == "start":
                c.start()
            elif mode == "send":
                c.wait_send()
            else:
                c.wait_recv()

    def advance(a, step):
        buf = pairs[a]
        from_l = buf.at[jnp.maximum(z - 1 - step, 0) * CORES + core]
        from_r = buf.at[jnp.minimum(z + 1 + step, depth - 1) * CORES + core]
        for way, ok, ref in ((0, z - 1 - step >= 0, from_l), (1, z + 1 + step < depth, from_r)):
            @pl.when(ok)
            def _(way=way, ref=ref):
                remote(ref, ref, z_send.at[a, way, step], z_recv.at[a, way, step],
                       "sp", lax.rem(mine + 1, groups)).wait_recv()
        if step + 1 < depth - 1:
            chain(a, step + 1)
        across(a, step + 1, 0, "start")
        across(a, step + 1, 1, "start")

    def settle(a):
        for step in range(depth - 1):
            chain(a, step, True)
        for step in range(depth):
            for way in range(2):
                if step or not way:
                    across(a, step, way, "send")

    def collected(a):
        for step in range(depth):
            for way in range(2):
                if step or not way:
                    across(a, step, way, "recv")

    loads[4].wait()
    chain(0, 0)
    across(0, 0, 0, "start")

    gathers = [[], []]

    def gather(a, src, dst):
        if chunked:
            for d in range(groups):
                at = lax.rem(mine + groups - d, groups)
                if d:
                    arrivals[a][d].wait_recv()
                for p in range(1, parts):
                    c = remote(dst.at[at, :, here] if d else src.at[mine], dst.at[at, :, here],
                               t_send.at[a, d, p], t_recv.at[a, d, p], "tp", lax.rem(col + p, parts))
                    c.start()
                    gathers[a].append(c)
            own[a].wait()
        else:
            own[a].wait()
            for d in range(1, groups):
                arrivals[a][d].wait_recv()
            for p in range(1, parts):
                c = remote(dst.at[:, :, here], dst.at[:, :, here],
                           t_send.at[a, 0, p], t_recv.at[a, 0, p], "tp", lax.rem(col + p, parts))
                c.start()
                gathers[a].append(c)
        sends.extend(gathers[a])

    gather(0, out_x, rows_x)
    loads[2].wait()
    loads[3].wait()
    act, branch_slope = gelu_parts(gate_ref[...].astype(F32))
    mix_own[...] = (act * states_ref[...]).astype(BF)
    gather(1, out_c, rows_c)
    o = pltpu.make_async_copy(mix_own, mixed_all.at[mine], w_sem.at[3])
    o.start()
    o.wait()
    for i in range(6, 9):
        loads[i].wait()
    for c in gathers[0]:
        c.wait_recv()
    row_data = rows_x[...].reshape(size, model)
    pre_gate = jnp.dot(row_data, wg[...], preferred_element_type=F32)
    pre_up = jnp.dot(row_data, wu[...], preferred_element_type=F32)
    active, slope = silu_parts(pre_gate)
    hidden = (active * pre_up).astype(BF)
    lean = pre_up * slope
    advance(0, 0)
    if depth > 2:
        advance(0, 1)
    for c in gathers[1]:
        c.wait_recv()
    grad_hidden = contract_cols(rows_c[...].reshape(size, model), wd[...])
    grad_pre_gate = (grad_hidden * lean).astype(BF)
    grad_pre_up = (grad_hidden * active).astype(BF)
    for d in list(range(1, parts)) + [0]:
        part = near(width, lax.rem(col + d, parts))
        term = contract_cols(grad_pre_gate, wg[part, :]) + contract_cols(grad_pre_up, wu[part, :])
        terms[d] = term.astype(BF).reshape(groups, room, width)

    share_copies = {}
    order = list(range(1, groups)) + [0]
    for d in order if chunked else [0]:
        at = lax.rem(mine + d, groups)
        for p in range(1, parts):
            src = terms.at[p, at] if chunked else terms.at[p]
            dst = shares.at[p - 1, at] if chunked else shares.at[p - 1]
            c = remote(src, dst, s_send.at[d, p], s_recv.at[d, p], "tp", lax.rem(col + p, parts))
            c.start()
            share_copies[d, p] = c
            sends.append(c)
    for step in range(2, depth - 1):
        advance(0, step)
    chain(1, 0)
    across(1, 0, 0, "start")

    stores = []

    def piece(kind, p):
        part = slice(p * width, (p + 1) * width)
        if kind == 2:
            gd[:, part] = contract_rows(hidden, rows_c[:, :, part].reshape(size, width)).astype(BF)
            s, t = gd.at[:, part], gd_ref.at[:, part]
        else:
            grad, buf, out = ((grad_pre_gate, gg, gg_ref), (grad_pre_up, gu, gu_ref))[kind]
            buf[part, :] = contract_rows(rows_x[:, :, part].reshape(size, width), grad).astype(BF)
            s, t = buf.at[part], out.at[part]
        o = pltpu.make_async_copy(s, t, w_sem.at[4 + kind * parts + p])
        o.start()
        stores.append(o)

    pieces = [(kind, p) for kind in range(3) for p in range(parts)]
    back_copies = []
    for d in order:
        if pieces:
            piece(*pieces.pop(0))
        at = lax.rem(mine + d, groups)
        if chunked or d == 1:
            for p in range(1, parts):
                share_copies[d if chunked else 0, p].wait_recv()
        total = terms[0, at].astype(F32)
        for p in range(1, parts):
            total = total + shares[p - 1, at].astype(F32)
        if d == 0:
            back[mine] = total.astype(BF)
        else:
            summed[d] = total.astype(BF)
            c = remote(summed.at[d], back.at[mine], r_send.at[d], r_recv.at[d], "sp", at)
            c.start()
            back_copies.append(c)
    nxt = lax.rem(mine + 1, groups)
    prev_copy = remote(states_ref.at[pl.ds(toks - 8, 8)], prev_in, p_send, p_recv, "sp", nxt)
    prev_copy.start()
    advance(1, 0)
    while pieces:
        piece(*pieces.pop(0))
    rows = lax.broadcasted_iota(jnp.int32, (toks, toks), 0)
    cols = lax.broadcasted_iota(jnp.int32, (toks, toks), 1)
    eye = jnp.where(rows == cols, 1.0, 0.0).astype(BF)
    total = contract_rows(cot_ref[...], eye)
    for c in back_copies:
        c.wait_recv()
    total = total + contract_rows(back[...].reshape(size, width), picked)
    flipped[here, :] = total.astype(BF)
    grad_copies = []
    for d in range(1, parts):
        part = flipped.at[here]
        c = remote(part, part, g_send.at[d], g_recv.at[d], "tp", lax.rem(col + d, parts))
        c.start()
        grad_copies.append(c)
    for step in range(1, depth - 1):
        advance(1, step)
    collected(0)
    loads[5].wait()
    for c in grad_copies:
        c.wait_recv()
    high = model // groups
    block_copies = []
    for d in range(1, groups):
        peer = lax.rem(mine + d, groups)
        c = remote(flipped.at[near(high, peer)], blocks.at[mine], b_send.at[d], b_recv.at[d], "sp", peer)
        c.start()
        block_copies.append(c)
    grad_mixed = contract_rows(flipped[...], proj_all[...].reshape(model, states_ref.shape[1]))
    states = states_ref[...]
    act, branch_slope = gelu_parts(gate_ref[...].astype(F32))
    decays = jnp.exp(decay_ref[...])
    ggate_ref[...] = (grad_mixed * states * branch_slope).astype(BF)
    local = grad_mixed * act
    line = lax.broadcasted_iota(jnp.int32, local.shape, 0)
    span = jnp.where(line < toks - 1, pltpu.roll(decays, toks - 1, 0), 1.0)
    k = 1
    while k < toks:
        inside = line < toks - k
        local = local + span * jnp.where(inside, pltpu.roll(local, toks - k, 0), 0.0)
        span = span * jnp.where(inside, pltpu.roll(span, toks - k, 0), 1.0)
        k *= 2
    eight = lax.broadcasted_iota(jnp.int32, (8, local.shape[1]), 0)
    whole = span[0:1] * decays[0:1]
    entry = local[0:1] * decays[0:1]
    carry_own[...] = jnp.where(eight == 0, whole, entry)
    carry_copies = []
    for d in range(1, groups):
        peer = lax.rem(mine + d, groups)
        c = remote(carry_own, carry_in.at[d - 1], k_send.at[d], k_recv.at[d], "sp", peer)
        c.start()
        carry_copies.append(c)
    collected(1)
    total = jnp.dot(flipped[near(high, mine), :], mixed_all[mine], preferred_element_type=F32)
    for d in range(1, groups):
        block_copies[d - 1].wait_recv()
        at = lax.rem(mine + groups - d, groups)
        total = total + jnp.dot(blocks[at], mixed_all[at], preferred_element_type=F32)
    outp_ref[...] = total
    prev_copy.wait_recv()
    first = jnp.where(mine > 0, prev_in[7:8, :], 0.0)
    prev = jnp.where(line == 0, first, pltpu.roll(states, 1, 0))
    for c in carry_copies:
        c.wait_recv()
    carried = jnp.zeros_like(whole)
    for ahead in range(groups - 1, 0, -1):
        got = carry_in[groups - ahead - 1]
        carried = jnp.where(mine + ahead < groups, got[1:2] + got[0:1] * carried, carried)
    grad_in = local + span * carried
    gin_ref[...] = grad_in
    gdecay_ref[...] = (grad_in * decays * prev).astype(BF)
    settle(0)
    settle(1)
    for c in [prev_copy] + sends + back_copies + grad_copies + block_copies + carry_copies:
        c.wait_send()
    for o in stores:
        o.wait()


def shards(
    moe_input, cotangent, routes, route_weights, gate_branch, log_decay, states,
    w_gate, w_up, w_down, out_proj,
):
    groups, parts = lax.axis_size("sp"), lax.axis_size("tp")
    tok_rows, picks = routes.shape
    width = moe_input.shape[1]
    model = width * parts
    units = w_gate.shape[2]
    chans = states.shape[1]
    room = tok_rows * picks * 5 // (4 * groups)
    room = (room + 7) // 8 * 8
    depth = groups // CORES
    high = out_proj.shape[0]
    chunked = groups * parts <= 64
    chunks = groups if chunked else 1
    vmem = pl.BlockSpec(memory_space=pltpu.VMEM)
    hbm = pl.BlockSpec(memory_space=pl.ANY)
    dma = pltpu.SemaphoreType.DMA

    def run(*refs):
        whole_kernel(groups, parts, room, chunked, *refs)

    def buf(*shape, kind=BF):
        return pltpu.VMEM(shape, kind)

    outs = pl.pallas_call(
        run,
        out_shape=[
            jax.ShapeDtypeStruct((model, units), BF),
            jax.ShapeDtypeStruct((model, units), BF),
            jax.ShapeDtypeStruct((units, model), BF),
            jax.ShapeDtypeStruct((high, chans), F32),
            jax.ShapeDtypeStruct((tok_rows, chans), BF),
            jax.ShapeDtypeStruct((tok_rows, chans), BF),
            jax.ShapeDtypeStruct((tok_rows, chans), F32),
        ],
        in_specs=[vmem] * 2 + [hbm] * 9,
        out_specs=[hbm] * 3 + [vmem] * 4,
        scratch_shapes=[
            buf(tok_rows, width), buf(tok_rows, width), buf(tok_rows, chans),
            buf(tok_rows, chans, kind=F32), buf(tok_rows, chans, kind=F32),
            buf(model, units), buf(model, units), buf(units, model),
            buf(groups, room, width), buf(groups, room, width),
            buf(groups, room, model), buf(groups, room, model),
            buf(groups, high, chans), buf(groups, tok_rows, chans), buf(tok_rows, chans),
            buf(model, units), buf(model, units), buf(units, model),
            buf(parts, groups, room, width), buf(parts - 1, groups, room, width),
            buf(groups, room, width), buf(groups, room, width),
            buf(model, tok_rows), buf(groups, high, tok_rows),
            buf(8, chans, kind=F32), buf(groups - 1, 8, chans, kind=F32), buf(8, chans, kind=F32),
        ]
        + [dma((2, groups))] * 2 + [dma((2, chunks, parts))] * 2 + [dma((2, 2, depth))] * 4
        + [dma((chunks, parts))] * 2 + [dma((groups,))] * 2 + [dma((parts,))] * 2
        + [dma((groups,))] * 4 + [dma(())] * 2 + [dma((9,)), dma((4 + 3 * parts,))],
        compiler_params=pltpu.CompilerParams(
            collective_id=0, has_side_effects=True, vmem_limit_bytes=60 * 1024 * 1024),
        name="backward",
    )(
        routes.T, route_weights.T, moe_input, cotangent, gate_branch, states, log_decay, out_proj,
        w_gate, w_up, w_down,
    )
    return tuple(out.astype(F32)[None] for out in outs[:3]) + tuple(outs[3:])


def solution(mesh):
    return jax.shard_map(
        shards,
        mesh=mesh,
        in_specs=(
            P("sp", "tp"), P("sp", "tp"), P("sp", None), P("sp", None), P("sp", "tp"),
            P("sp", "tp"), P("sp", "tp"), P("sp", None, "tp"), P("sp", None, "tp"),
            P("sp", "tp", None), P("sp", "tp"),
        ),
        out_specs=(
            P("sp", None, "tp"), P("sp", None, "tp"), P("sp", "tp", None), P("sp", "tp"),
            P("sp", "tp"), P("sp", "tp"), P("sp", "tp"),
        ),
        check_vma=False,
    )
```
